128 devices in a mesh: fs: 16 (over z, y), tp: 8 (over x, core).
Axes of the slice: x: 4, y: 4, z: 4, core: 2. Of those that a mesh axis runs over, the one named last changes fastest.
Arguments:
- layer_input: bfloat16 [40960, 4096], P('fs'), may hold values from -140 to 140
- query_cotangent: bfloat16 [40960, 2048], P('fs', 'tp'), may hold values from -0.33105094 to 0.33105094
- value_cotangent: bfloat16 [40960, 512], P('fs', 'tp'), may hold values from -0.33105094 to 0.33105094
- query_weight: float32 [4096, 2048], P('fs', 'tp'), may hold values from -0.09375 to 0.09375
- value_weight: float32 [4096, 512], P('fs', 'tp'), may hold values from -0.09375 to 0.09375
- query_moment: float32 [4096, 2048], P('fs', 'tp'), may hold values from -18 to 18
- value_moment: float32 [4096, 512], P('fs', 'tp'), may hold values from -18 to 18
- query_left_stat: float32 [16, 256, 256], P('fs'), may hold values from -24 to 24
- value_left_stat: float32 [16, 256, 256], P('fs'), may hold values from -24 to 24
- query_right_stat: float32 [32, 64, 64], P('tp'), may hold values from -24 to 24
- value_right_stat: float32 [8, 64, 64], P('tp'), may hold values from -24 to 24
- query_left_root: bfloat16 [16, 256, 256], P('fs'), may hold values from -1.5 to 2
- value_left_root: bfloat16 [16, 256, 256], P('fs'), may hold values from -1.5 to 2
- query_right_root: bfloat16 [32, 64, 64], P('tp'), may hold values from -1.5 to 2
- value_right_root: bfloat16 [8, 64, 64], P('tp'), may hold values from -1.5 to 2
Outputs:
- query_update: float32 [4096, 2048], P('fs', 'tp')
- value_update: float32 [4096, 512], P('fs', 'tp')
- query_moment_new: float32 [4096, 2048], P('fs', 'tp')
- value_moment_new: float32 [4096, 512], P('fs', 'tp')
- query_left_new: float32 [16, 256, 256], P('fs')
- value_left_new: float32 [16, 256, 256], P('fs')
- query_right_new: float32 [32, 64, 64], P('tp')
- value_right_new: float32 [8, 64, 64], P('tp')
- query_copy: bfloat16 [4096, 2048], P(None, 'tp')
- value_copy: bfloat16 [4096, 512], P(None, 'tp')
The draws below stay inside these ranges and needn't reach their ends.
All inputs are finite; a program needn't handle non-finite values.
Results may differ from the reference program's by a relative error of at most 0.0075.
Values may be sent and summed in bfloat16 or wider, within the bound.
No kernel may reach another device: no remote copies, remote signals or barrier semaphores. Data moves between devices by JAX's collectives and lax.ppermute only.
A program may use at most 128 MiB of HBM per device.

```python
import jax
import jax.numpy as jnp
from jax import lax

D = 4096
HEADS = 32
KV_HEADS = 8
HEAD = 64
BLOCK = 256
TOKENS = 40960
Q_COLS = 2048
V_COLS = 512


def scaled_draw(key, row_count, columns, base_scale):
    noise_key, scale_key = jax.random.split(key, 2)
    column_ramp = jnp.arange(columns, dtype=jnp.float32) / columns
    jitter = jax.random.uniform(scale_key, (columns,), jnp.float32)
    noise = jnp.clip(jax.random.normal(noise_key, (row_count, columns), jnp.float32), -6.0, 6.0)
    exponent = 0.5 * column_ramp + 0.5 * jitter
    return (noise * (base_scale * 10.0 ** exponent)).astype(jnp.bfloat16)


def root_draw(key, matrix_count, order):
    diag_key, off_key = jax.random.split(key, 2)
    diagonal = jax.random.uniform(diag_key, (matrix_count, order), jnp.float32, 0.6, 1.4)
    spread = jnp.clip(jax.random.normal(off_key, (matrix_count, order, order), jnp.float32), -4.0, 4.0)
    spread = spread * (0.6 / order ** 0.5)
    spread = 0.5 * (spread + jnp.swapaxes(spread, 1, 2))
    identity = jnp.eye(order, dtype=jnp.float32)
    return (spread * (1.0 - identity) + diagonal[:, :, None] * identity).astype(jnp.bfloat16)


def draw_layer_input(key, part):
    return scaled_draw(jax.random.fold_in(key, 11), TOKENS, D, 1.0)


def draw_query_cotangent(key, part):
    return scaled_draw(jax.random.fold_in(key, 12), TOKENS, Q_COLS, 0.5 / TOKENS ** 0.5)


def draw_value_cotangent(key, part):
    return scaled_draw(jax.random.fold_in(key, 13), TOKENS, V_COLS, 0.5 / TOKENS ** 0.5)


def draw_query_left_root(key, part):
    return root_draw(jax.random.fold_in(key, 21), D // BLOCK, BLOCK)


def draw_value_left_root(key, part):
    return root_draw(jax.random.fold_in(key, 22), D // BLOCK, BLOCK)


def draw_query_right_root(key, part):
    return root_draw(jax.random.fold_in(key, 23), HEADS, HEAD)


def draw_value_right_root(key, part):
    return root_draw(jax.random.fold_in(key, 24), KV_HEADS, HEAD)


def levels(rng, extent, shards, least, top_value):
    def one(dim, shards_of):
        steps = jax.random.uniform(jax.random.fold_in(jax.random.fold_in(rng, 6), dim), (shards_of,), jnp.float32, least / len(shards), top_value / len(shards))
        return jnp.repeat(jnp.exp(steps), extent[dim] // shards_of).reshape((-1,) + (1,) * (len(extent) - dim - 1))

    level = one(*shards[0])
    for cut in shards[1:]:
        level = level * one(*cut)
    return level


def normal_values(own_key, dims, width, reach, shards=(), held_as=jnp.bfloat16):
    result = width * jax.random.normal(own_key, dims, jnp.float32)
    if shards:
        result = result * levels(own_key, dims, shards, -0.22, 0.18)
    return jnp.clip(result, -reach, reach).astype(held_as)


def setup_inputs(seed: int = 0) -> dict:
    keys = jax.random.split(jax.random.key(seed), 16)
    layer_input = draw_layer_input(jax.random.fold_in(keys[15], 71), 0)
    query_cotangent = draw_query_cotangent(jax.random.fold_in(keys[15], 71), 0)
    value_cotangent = draw_value_cotangent(jax.random.fold_in(keys[15], 71), 0)
    query_weight = normal_values(keys[3], (D, Q_COLS), D ** -0.5, 0.09375, ((0, 16), (1, 8)), jnp.float32)
    value_weight = normal_values(keys[4], (D, V_COLS), D ** -0.5, 0.09375, ((0, 16), (1, 8)), jnp.float32)
    query_moment = normal_values(keys[5], (D, Q_COLS), 3.0, 18.0, ((0, 16), (1, 8)), jnp.float32)
    value_moment = normal_values(keys[6], (D, V_COLS), 3.0, 18.0, ((0, 16), (1, 8)), jnp.float32)
    query_left_stat = normal_values(keys[7], (D // BLOCK, BLOCK, BLOCK), 4.0, 24.0, ((0, 16),), jnp.float32)
    value_left_stat = normal_values(keys[8], (D // BLOCK, BLOCK, BLOCK), 4.0, 24.0, ((0, 16),), jnp.float32)
    query_right_stat = normal_values(keys[9], (HEADS, HEAD, HEAD), 4.0, 24.0, ((0, 8),), jnp.float32)
    value_right_stat = normal_values(keys[10], (KV_HEADS, HEAD, HEAD), 4.0, 24.0, ((0, 8),), jnp.float32)
    query_left_root = draw_query_left_root(jax.random.fold_in(keys[15], 71), 0)
    value_left_root = draw_value_left_root(jax.random.fold_in(keys[15], 71), 0)
    query_right_root = draw_query_right_root(jax.random.fold_in(keys[15], 71), 0)
    value_right_root = draw_value_right_root(jax.random.fold_in(keys[15], 71), 0)
    return {"layer_input": layer_input, "query_cotangent": query_cotangent, "value_cotangent": value_cotangent, "query_weight": query_weight, "value_weight": value_weight, "query_moment": query_moment, "value_moment": value_moment, "query_left_stat": query_left_stat, "value_left_stat": value_left_stat, "query_right_stat": query_right_stat, "value_right_stat": value_right_stat, "query_left_root": query_left_root, "value_left_root": value_left_root, "query_right_root": query_right_root, "value_right_root": value_right_root}


momentum_decay = 0.9
statistic_decay = 0.9
learning_rate = 0.002
epsilon = 1e-06
highest = lax.Precision.HIGHEST

def token_sum(inputs, cotangent):
    return lax.dot_general(inputs, cotangent, (((0,), (0,)), ((), ())), preferred_element_type=jnp.float32)

def precondition(moment, left_root, right_root):
    total_rows, columns = moment.shape
    head_count = columns // HEAD
    by_head = jnp.einsum('rhk,hkl->rhl', moment.reshape(total_rows, head_count, HEAD), right_root.astype(jnp.float32), precision=highest)
    by_block = by_head.reshape(total_rows // BLOCK, BLOCK, columns)
    return jnp.einsum('bij,bjc->bic', left_root.astype(jnp.float32), by_block, precision=highest).reshape(total_rows, columns)

def update_matrix(gradient, weight, moment, left_stat, right_stat, left_root, right_root):
    total_rows, columns = gradient.shape
    moment_new = momentum_decay * moment + (1.0 - momentum_decay) * gradient
    blocks = gradient.reshape(total_rows // BLOCK, BLOCK, columns)
    left_sum = jnp.einsum('bic,bjc->bij', blocks, blocks, precision=highest)
    left_new = statistic_decay * left_stat + (1.0 - statistic_decay) / columns * left_sum
    per_head = gradient.reshape(total_rows, columns // HEAD, HEAD)
    right_sum = jnp.einsum('rhk,rhl->hkl', per_head, per_head, precision=highest)
    right_new = statistic_decay * right_stat + (1.0 - statistic_decay) / total_rows * right_sum
    direction = precondition(moment_new, left_root, right_root)
    graft_scale = jnp.sqrt(jnp.sum(moment_new * moment_new) / (jnp.sum(direction * direction) + epsilon))
    update = graft_scale * direction
    weight_copy = (weight - learning_rate * update).astype(jnp.bfloat16)
    return (update, moment_new, left_new, right_new, weight_copy)

def reference(layer_input, query_cotangent, value_cotangent, query_weight, value_weight, query_moment, value_moment, query_left_stat, value_left_stat, query_right_stat, value_right_stat, query_left_root, value_left_root, query_right_root, value_right_root):
    query_gradient = token_sum(layer_input, query_cotangent)
    value_gradient = token_sum(layer_input, value_cotangent)
    query_parts = update_matrix(query_gradient, query_weight, query_moment, query_left_stat, query_right_stat, query_left_root, query_right_root)
    value_parts = update_matrix(value_gradient, value_weight, value_moment, value_left_stat, value_right_stat, value_left_root, value_right_root)
    return (query_parts[0], value_parts[0], query_parts[1], value_parts[1], query_parts[2], value_parts[2], query_parts[3], value_parts[3], query_parts[4], value_parts[4])
```

```python
import functools

import jax
import jax.numpy as jnp
from jax import lax
from jax.experimental import pallas as pl
from jax.experimental.pallas import tpu as pltpu
from jax.sharding import PartitionSpec as P

D = 4096
HEAD = 64
BLOCK = 256
Q_COLS = 2048
V_COLS = 512
QW = 256
VW = 64
W = QW + VW
RW = 80

momentum_decay = 0.9
statistic_decay = 0.9
learning_rate = 0.002
epsilon = 1e-06


AXES = ("fs", "tp")
f32 = jnp.float32
bf16 = jnp.bfloat16
VM = pl.BlockSpec(memory_space=pltpu.VMEM)


def device(z, y, x, c):
    return ((z * 4 + y) * 4 + x) * 2 + c


def every_device():
    return [
        (z, y, x, c) for z in range(4) for y in range(4) for x in range(4) for c in range(2)
    ]


def shift_line(value, step, first):
    pairs = []
    for z, y, x, c in every_device():
        along_z = (c == 0) == first
        to = ((z + step) % 4, y) if along_z else (z, (y + step) % 4)
        pairs.append((device(z, y, x, c), device(*to, x, c)))
    return lax.ppermute(value, AXES, pairs)


def shift_x(value, step):
    pairs = [(device(z, y, x, c), device(z, y, (x + step) % 4, c)) for z, y, x, c in every_device()]
    return lax.ppermute(value, AXES, pairs)


def swap_cores(value):
    pairs = [(device(z, y, x, c), device(z, y, x, 1 - c)) for z, y, x, c in every_device()]
    return lax.ppermute(value, AXES, pairs)


def dot(a, b, ca=1, cb=0):
    return lax.dot_general(a, b, (((ca,), (cb,)), ((), ())), preferred_element_type=f32)


def split(a):
    hi = a.astype(bf16)
    return hi, (a - hi.astype(f32)).astype(bf16)


def token_kernel(blk, cot, x, out):
    out[0] = dot(cot[...], x[...]).astype(bf16)


def token_sums(blk, cot_t, layer_input, chunk):
    tokens = layer_input.shape[0]
    return pl.pallas_call(
        token_kernel,
        out_shape=jax.ShapeDtypeStruct((4, W, BLOCK), bf16),
        grid_spec=pltpu.PrefetchScalarGridSpec(
            num_scalar_prefetch=1,
            grid=(4,),
            in_specs=[
                pl.BlockSpec((W, tokens), lambda k, b: (0, 0)),
                pl.BlockSpec((tokens, BLOCK), lambda k, b: (0, b[4 * chunk + k])),
            ],
            out_specs=pl.BlockSpec((1, W, BLOCK), lambda k, b: (k, 0, 0)),
        ),
        compiler_params=pltpu.CompilerParams(vmem_limit_bytes=52 << 20),
        cost_estimate=pl.CostEstimate(
            flops=2 * 4 * W * BLOCK * tokens,
            bytes_accessed=2 * (4 * BLOCK * tokens + W * tokens),
            transcendentals=0,
        ),
        name="token_sums",
    )(blk, cot_t, layer_input)


def local_kernel(
    own, r1, r2, r3, q_mom, v_mom, q_lroot, v_lroot, q_rroot, v_rroot,
    q_mnew, v_mnew, q_dir, v_dir, left, right, squares,
):
    gt = own[...].astype(f32) + r1[...].astype(f32) + r2[...].astype(f32) + r3[...].astype(f32)
    gq_t = gt[:QW]
    gv_t = gt[QW:]
    gq = gq_t.T
    mq = momentum_decay * q_mom[...] + (1.0 - momentum_decay) * gq
    mv = momentum_decay * v_mom[...] + (1.0 - momentum_decay) * gv_t
    q_mnew[...] = mq
    v_mnew[...] = mv
    rows = []
    for h in range(QW // HEAD):
        rr = q_rroot[h]
        parts = [jnp.zeros((HEAD, HEAD), bf16)] * h + [rr] + [jnp.zeros((HEAD, HEAD), bf16)] * (3 - h)
        rows.append(jnp.concatenate(parts, axis=1))
    rbd = jnp.concatenate(rows, axis=0)
    mq_hi, mq_lo = split(mq)
    tq_hi, tq_lo = split(dot(mq_hi, rbd) + dot(mq_lo, rbd))
    lq = q_lroot[0]
    dq = dot(lq, tq_hi) + dot(lq, tq_lo)
    q_dir[...] = dq
    mv_hi, mv_lo = split(mv)
    rv = v_rroot[0]
    tv_hi, tv_lo = split(dot(rv, mv_hi, 0, 0) + dot(rv, mv_lo, 0, 0))
    lv = v_lroot[0]
    dv = dot(tv_hi, lv, 1, 1) + dot(tv_lo, lv, 1, 1)
    v_dir[...] = dv
    lane = lax.broadcasted_iota(jnp.int32, (128, 128), 1)
    sums = [jnp.sum(mq * mq), jnp.sum(dq * dq), jnp.sum(mv * mv), jnp.sum(dv * dv)]
    row = jnp.zeros((128, 128), f32)
    for i, s in enumerate(sums):
        row = jnp.where(lane == i, s, row)
    squares[...] = row
    gq_hi, gq_lo = split(gq)
    lp = dot(gq_hi, gq_hi, 1, 1) + dot(gq_hi, gq_lo, 1, 1) + dot(gq_lo, gq_hi, 1, 1)
    left[0] = lp.astype(bf16)
    gv = gv_t.T
    gv_hi, gv_lo = split(gv)
    lp = dot(gv_hi, gv_hi, 1, 1) + dot(gv_hi, gv_lo, 1, 1) + dot(gv_lo, gv_hi, 1, 1)
    left[1] = lp.astype(bf16)
    gt_hi, gt_lo = split(gq_t)
    rp = dot(gt_hi, gt_hi, 1, 1) + dot(gt_hi, gt_lo, 1, 1) + dot(gt_lo, gt_hi, 1, 1)
    head = lax.broadcasted_iota(jnp.int32, (HEAD, QW), 1) // HEAD
    packed = jnp.zeros((HEAD, QW), f32)
    for h in range(QW // HEAD):
        packed = jnp.where(head == h, rp[HEAD * h : HEAD * (h + 1)], packed)
    gvt_hi, gvt_lo = split(gv_t)
    vp = dot(gvt_hi, gvt_hi, 1, 1) + dot(gvt_hi, gvt_lo, 1, 1) + dot(gvt_lo, gvt_hi, 1, 1)
    vp = vp.astype(bf16)
    src = lax.broadcasted_iota(jnp.int32, (HEAD, QW), 0)
    dst = lax.broadcasted_iota(jnp.int32, (HEAD, QW), 1)
    vpacked = jnp.zeros((16, QW), f32)
    for j in range(4):
        place = (dst == src + HEAD * j).astype(bf16)
        vpacked = vpacked + dot(vp[16 * j : 16 * (j + 1)], place)
    right[:HEAD] = packed.astype(bf16)
    right[HEAD:] = vpacked.astype(bf16)


def local_work(*args):
    shapes = [
        ((BLOCK, QW), f32), ((VW, BLOCK), f32), ((BLOCK, QW), f32), ((VW, BLOCK), f32),
        ((2, BLOCK, BLOCK), bf16), ((RW, QW), bf16), ((128, 128), f32),
    ]
    return pl.pallas_call(
        local_kernel,
        out_shape=[jax.ShapeDtypeStruct(s, t) for s, t in shapes],
        in_specs=[VM] * 10,
        out_specs=[VM] * 7,
        compiler_params=pltpu.CompilerParams(vmem_limit_bytes=24 << 20),
        cost_estimate=pl.CostEstimate(
            flops=2 * 20 * 256**3, bytes_accessed=4 << 20, transcendentals=0
        ),
        name="local_work",
    )(*args)


def update_kernel(squares, q_dir, v_dir, q_w, v_w, right, q_up, v_up, message):
    total = jnp.sum(squares[...], axis=0, keepdims=True)
    lane = lax.broadcasted_iota(jnp.int32, (1, 128), 1)
    s = [jnp.sum(jnp.where(lane == i, total, 0.0), axis=1, keepdims=True) for i in range(4)]
    uq = jnp.sqrt(s[0] / (s[1] + epsilon)) * q_dir[...]
    uv = jnp.sqrt(s[2] / (s[3] + epsilon)) * v_dir[...]
    q_up[...] = uq
    v_up[...] = uv
    message[:BLOCK] = (q_w[...] - learning_rate * uq).astype(bf16)
    message[BLOCK:W] = (v_w[...] - learning_rate * uv).astype(bf16)
    message[W:] = right[...]


def updates(*args):
    shapes = [((BLOCK, QW), f32), ((VW, BLOCK), f32), ((W + RW, QW), bf16)]
    return pl.pallas_call(
        update_kernel,
        out_shape=[jax.ShapeDtypeStruct(s, t) for s, t in shapes],
        in_specs=[VM] * 6,
        out_specs=[VM] * 3,
        compiler_params=pltpu.CompilerParams(vmem_limit_bytes=16 << 20),
        cost_estimate=pl.CostEstimate(flops=1 << 20, bytes_accessed=2 << 20, transcendentals=0),
        name="updates",
    )(*args)


def stack_kernel(m0, m1, m2, m3, out):
    total = jnp.zeros((RW, QW), f32)
    for k, m in enumerate((m0, m1, m2, m3)):
        out[W * k : W * (k + 1)] = m[:W]
        total = total + m[W:].astype(f32)
    out[4 * W :] = total.astype(bf16)


def stack_blocks(*args):
    return pl.pallas_call(
        stack_kernel,
        out_shape=jax.ShapeDtypeStruct((4 * W + RW, QW), bf16),
        in_specs=[VM] * 4,
        out_specs=VM,
        compiler_params=pltpu.CompilerParams(vmem_limit_bytes=16 << 20),
        cost_estimate=pl.CostEstimate(flops=1 << 18, bytes_accessed=2 << 20, transcendentals=0),
        name="stack_blocks",
    )(*args)


def place_kernel(where, m0, m1, m2, m3, q_rstat, v_rstat, q_copy, v_copy, q_rnew, v_rnew, sem):
    copies = []
    for j, m in enumerate((m0, m1, m2, m3)):
        for k in range(4):
            row = pl.multiple_of(where[4 * j + k] * BLOCK, BLOCK)
            copies.append(
                pltpu.make_async_copy(
                    m.at[pl.ds(W * k, BLOCK)], q_copy.at[pl.ds(row, BLOCK)], sem.at[0, 4 * j + k]
                )
            )
            copies.append(
                pltpu.make_async_copy(
                    m.at[pl.ds(W * k + BLOCK, VW)],
                    v_copy.at[:, pl.ds(row, BLOCK)],
                    sem.at[1, 4 * j + k],
                )
            )
    for c in copies:
        c.start()
    total = jnp.zeros((RW, QW), f32)
    for m in (m0, m1, m2, m3):
        total = total + m[4 * W :].astype(f32)
    total = (1.0 - statistic_decay) / D * total
    for h in range(4):
        part = slice(HEAD * h, HEAD * (h + 1))
        q_rnew[h] = statistic_decay * q_rstat[h] + total[:HEAD, part]
        rows = slice(16 * h, 16 * (h + 1))
        v_rnew[0, rows] = statistic_decay * v_rstat[0, rows] + total[HEAD:, part]
    for c in copies:
        c.wait()


def place_blocks(where, *args):
    return pl.pallas_call(
        place_kernel,
        out_shape=[
            jax.ShapeDtypeStruct((D, QW), bf16),
            jax.ShapeDtypeStruct((VW, D), bf16),
            jax.ShapeDtypeStruct((4, HEAD, HEAD), f32),
            jax.ShapeDtypeStruct((1, HEAD, HEAD), f32),
        ],
        in_specs=[pl.BlockSpec(memory_space=pltpu.SMEM)] + [VM] * 6,
        out_specs=[pl.BlockSpec(memory_space=pl.ANY), pl.BlockSpec(memory_space=pl.ANY), VM, VM],
        scratch_shapes=[pltpu.SemaphoreType.DMA((2, 16))],
        compiler_params=pltpu.CompilerParams(vmem_limit_bytes=16 << 20),
        cost_estimate=pl.CostEstimate(flops=1 << 18, bytes_accessed=6 << 20, transcendentals=0),
        name="place_blocks",
    )(where, *args)


def local(
    layer_input,
    query_cotangent,
    value_cotangent,
    query_weight,
    value_weight,
    query_moment,
    value_moment,
    query_left_stat,
    value_left_stat,
    query_right_stat,
    value_right_stat,
    query_left_root,
    value_left_root,
    query_right_root,
    value_right_root,
):
    fs, tp = lax.axis_index("fs"), lax.axis_index("tp")
    core = tp % 2
    line = jnp.where(core == 0, fs // 4, fs % 4)
    other = jnp.where(core == 0, fs % 4, fs // 4)
    line_stride = jnp.where(core == 0, 4, 1)
    other_stride = 5 - line_stride
    steps = jnp.array([2, 1, 3, 0], jnp.int32)[:, None]
    ks = jnp.arange(4, dtype=jnp.int32)[None, :]
    blk = ((line + steps) % 4 * line_stride + (other + ks) % 4 * other_stride).reshape(16)
    cot_t = jnp.concatenate([query_cotangent.T, value_cotangent.T], axis=0)

    part2 = token_sums(blk, cot_t, layer_input, 0)
    got2 = shift_line(part2, 2, True)
    part1 = token_sums(blk, cot_t, layer_input, 1)
    got1 = shift_line(part1, 1, True)
    part3 = token_sums(blk, cot_t, layer_input, 2)
    got3 = shift_line(part3, 3, True)
    part0 = token_sums(blk, cot_t, layer_input, 3)
    half = (
        part0.astype(f32) + got2.astype(f32) + got1.astype(f32) + got3.astype(f32)
    ).astype(bf16)
    recv = [shift_line(half[k], k, False) for k in (2, 1, 3)]

    q_mnew, v_mnew, q_dir, v_dir, left, right, squares = local_work(
        half[0], *recv, query_moment, value_moment.T, query_left_root, value_left_root,
        query_right_root, value_right_root,
    )
    squares = lax.all_to_all(squares, AXES, 0, 0, tiled=True)
    q_up, v_up, message = updates(squares, q_dir, v_dir, query_weight, value_weight.T, right)
    message, left = lax.optimization_barrier((message, left))
    first = [shift_line(message, k, False) for k in (2, 1, 3)]
    stacked = stack_blocks(message, *first)
    second = [shift_line(stacked, k, True) for k in (2, 1, 3)]
    back = jnp.array([0, 2, 1, 3], jnp.int32)
    where = (
        (line - back[:, None] + 4) % 4 * line_stride + (other - back[None, :] + 4) % 4 * other_stride
    ).reshape(16)
    q_copy, v_copy, q_right_new, v_right_new = place_blocks(
        where, stacked, *second, query_right_stat, value_right_stat
    )

    over_x = [shift_x(left, k) for k in (2, 1, 3)]
    left_x = (
        left.astype(f32) + over_x[0].astype(f32) + over_x[1].astype(f32) + over_x[2].astype(f32)
    ).astype(bf16)
    left_all = left_x.astype(f32) + swap_cores(left_x).astype(f32)
    q_left_new = statistic_decay * query_left_stat + (1.0 - statistic_decay) / Q_COLS * left_all[:1]
    v_left_new = statistic_decay * value_left_stat + (1.0 - statistic_decay) / V_COLS * left_all[1:]
    return (
        q_up, v_up.T, q_mnew, v_mnew.T, q_left_new, v_left_new, q_right_new, v_right_new,
        q_copy, v_copy.T,
    )


def solution(mesh):
    placed = (
        P("fs", None),
        P("fs", "tp"),
        P("fs", "tp"),
        P("fs", "tp"),
        P("fs", "tp"),
        P("fs", "tp"),
        P("fs", "tp"),
        P("fs", None, None),
        P("fs", None, None),
        P("tp", None, None),
        P("tp", None, None),
        P("fs", None, None),
        P("fs", None, None),
        P("tp", None, None),
        P("tp", None, None),
    )
    return jax.shard_map(
        local,
        mesh=mesh,
        in_specs=placed,
        out_specs=(
            P("fs", "tp"),
            P("fs", "tp"),
            P("fs", "tp"),
            P("fs", "tp"),
            P("fs", None, None),
            P("fs", None, None),
            P("tp", None, None),
            P("tp", None, None),
            P(None, "tp"),
            P(None, "tp"),
        ),
        check_vma=False,
    )
```
